32 devices in a mesh: fs: 4 (over y, x), tp: 8 (over z, core).
Axes of the slice: x: 2, y: 2, z: 4, core: 2. Of those that a mesh axis runs over, the one named last changes fastest.
Arguments:
- tokens: bfloat16 [512, 4096], P('fs', 'tp'), may hold values from -6 to 6
- expert_ids: int32 [512, 8], P('fs'), may hold values from 0 to 63, all different within a row; in each aligned block of 128 rows (0 to 127, 128 to 255, ...) at most 32 rows name the same one
- affinity: float32 [512, 8], P('fs'), may hold values from 0.05 to 1
- norm_gain: float32 [4096], P('fs'), may hold values from 0.1 to 1.9
- gate_train: float32 [64, 512, 4096], P(None, 'tp', 'fs'), may hold values from -0.09375 to 0.09375
- up_train: float32 [64, 512, 4096], P(None, 'tp', 'fs'), may hold values from -0.09375 to 0.09375
- down_train: float32 [64, 512, 4096], P(None, 'fs', 'tp'), may hold values from -0.25 to 0.25
- shared_gate_train: float32 [512, 4096], P('tp', 'fs'), may hold values from -0.09375 to 0.09375
- shared_up_train: float32 [512, 4096], P('tp', 'fs'), may hold values from -0.09375 to 0.09375
- shared_down_train: float32 [512, 4096], P('fs', 'tp'), may hold values from -0.25 to 0.25
Outputs:
- mixed: bfloat16 [512, 4096], P('fs', 'tp')
- gate_serve: bfloat16 [64, 512, 4096], P('fs', 'tp')
- up_serve: bfloat16 [64, 512, 4096], P('fs', 'tp')
- down_serve: bfloat16 [64, 512, 4096], P('fs', None, 'tp')
- shared_gate_serve: bfloat16 [512, 4096], P('tp')
- shared_up_serve: bfloat16 [512, 4096], P('tp')
- shared_down_serve: bfloat16 [512, 4096], P(None, 'tp')
The draws below stay inside these ranges and needn't reach their ends.
Inputs may be any that keep to these rules, and one draw needn't show every extreme that they name: `expert_ids`: each row names 8 different experts. In each aligned block of 128 rows (the tokens of one index of fs) no expert is named by more than 32 rows, a bound that some block reaches.
All inputs are finite; a program needn't handle non-finite values.
Results may differ from the reference program's by a relative error of at most 0.019.
Values may be sent and summed in bfloat16 or wider, within the bound.
A program may use at most 192 MiB of HBM per device.

```python
import math
import jax
import jax.numpy as jnp
import numpy as np
from jax import lax

D = 4096
H = 512
EXPERTS = 64
K = 8
TOK = 128
CAP = 32
TOKENS = 512
N_FS = 4


def block_scale(own_key, dims, cuts, smallest, high):
    level = 1.0
    for dim, shards_of in cuts:
        heights = jax.random.uniform(jax.random.fold_in(jax.random.fold_in(own_key, 6), dim), (shards_of,), jnp.float32, smallest / len(cuts), high / len(cuts))
        level = level * jnp.repeat(jnp.exp(heights), dims[dim] // shards_of).reshape((-1,) + (1,) * (len(dims) - 1 - dim))
    return level


def assign_block(stream_key, own, number, rows, amount, top, reach, lean):
    order = jax.random.permutation(stream_key, amount)
    packed, usual = shares(amount, rows * top, reach, lean, True), shares(amount, rows * top, reach, lean, False)
    places = jnp.arange(amount)

    def named(tallies, rotation):
        used = int((tallies > 0).sum())
        fixed = max(1, used // 4)
        moved = fixed + (places - fixed + rotation * (used - fixed)) % max(1, amount - fixed)
        return jnp.zeros((amount,), jnp.int32).at[order[jnp.where(places < fixed, places, moved)]].set(jnp.asarray(tallies, jnp.int32))

    tallies = jnp.where(number % 4 == 0, named(packed, number // 4), named(usual, number - number // 4 - 1))
    mixed = jax.random.permutation(jax.random.fold_in(own, 3), amount)
    giver, taker = mixed[0:amount // 2 * 2:2], mixed[1:amount // 2 * 2:2]
    slack = jnp.minimum(tallies[giver] - 1, reach - tallies[taker]) // 2
    slack = jnp.where((giver == order[0]) | (taker == order[0]) | (tallies[taker] == 0), 0, jnp.maximum(slack, 0))
    moved = jax.random.randint(jax.random.fold_in(own, 4), (amount // 2,), 0, 1 << 20) % (slack + 1)
    tallies = tallies.at[giver].add(-moved).at[taker].add(moved)
    items = jnp.searchsorted(jnp.cumsum(tallies), jnp.arange(rows * top), side="right").astype(jnp.int32)
    table = items.reshape(top, rows).T
    table = table[jax.random.permutation(jax.random.fold_in(own, 1), rows)]
    rotation = jax.random.randint(jax.random.fold_in(own, 2), (rows, 1), 0, top)
    return jnp.take_along_axis(table, (jnp.arange(top)[None, :] + rotation) % top, axis=1)


def shares(count, total, limit, lean, full):
    portions = [(1 << 20) // math.isqrt(rank ** lean) + 1 for rank in range(1, count + 1)]
    largest = limit if full else min(limit, max(-(-total // count), total * portions[0] // sum(portions)))
    least = 1 if total - largest >= count - 1 else 0
    holding, spare = [largest] + [least] * (count - 1), total - largest - least * (count - 1)
    while spare > 0:
        free = [i for i in range(1, count) if holding[i] < largest] or [i for i in range(1, count) if holding[i] < limit]
        whole, left = sum([portions[i] for i in free]), spare
        for i in free:
            more = min(limit - holding[i], max(1, left * portions[i] // whole), spare)
            holding[i] = holding[i] + more
            spare = spare - more
    return np.array(holding)


def bell_draw(key, extent, scale, limit, pieces=(), kind=jnp.bfloat16):
    result = scale * jax.random.normal(key, extent, jnp.float32)
    if pieces:
        result = result * block_scale(key, extent, pieces, -0.22, 0.18)
    return jnp.clip(result, -limit, limit).astype(kind)


def setup_inputs(seed: int = 0) -> dict:
    seeds = jax.random.split(jax.random.key(seed), 11)
    tokens = bell_draw(seeds[0], (TOKENS, D), 1.0, 6.0, ((0, 4), (1, 8)))
    expert_ids_keys = jax.random.split(jax.random.fold_in(seeds[1], 1), TOKENS // TOK)
    expert_ids_turns = jax.random.permutation(jax.random.fold_in(seeds[1], 3), TOKENS // TOK)
    expert_ids = jax.vmap(lambda own, number: assign_block(jax.random.fold_in(seeds[1], 2), own, number, TOK, EXPERTS, K, CAP, 1))(expert_ids_keys, expert_ids_turns).reshape((TOKENS, K))
    affinity = jnp.clip(0.05 + 0.95 * jax.random.uniform(seeds[2], (TOKENS, K), jnp.float32) ** block_scale(seeds[2], (TOKENS, K), ((0, 4),), -0.2, 0.2), 0.05, 1.0)
    norm_gain = jnp.clip(1.0 + 0.18 * jax.random.normal(seeds[3], (D,), jnp.float32), 0.1, 1.9)
    gate_train = bell_draw(seeds[4], (EXPERTS, H, D), D ** -0.5, 0.09375, ((1, 8), (2, 4)), jnp.float32)
    up_train = bell_draw(seeds[5], (EXPERTS, H, D), D ** -0.5, 0.09375, ((1, 8), (2, 4)), jnp.float32)
    down_train = bell_draw(seeds[6], (EXPERTS, H, D), H ** -0.5, 0.25, ((1, 4), (2, 8)), jnp.float32)
    shared_gate_train = bell_draw(seeds[7], (H, D), D ** -0.5, 0.09375, ((0, 8), (1, 4)), jnp.float32)
    shared_up_train = bell_draw(seeds[8], (H, D), D ** -0.5, 0.09375, ((0, 8), (1, 4)), jnp.float32)
    shared_down_train = bell_draw(seeds[9], (H, D), H ** -0.5, 0.25, ((0, 4), (1, 8)), jnp.float32)
    return {"tokens": tokens, "expert_ids": expert_ids, "affinity": affinity, "norm_gain": norm_gain, "gate_train": gate_train, "up_train": up_train, "down_train": down_train, "shared_gate_train": shared_gate_train, "shared_up_train": shared_up_train, "shared_down_train": shared_down_train}


norm_eps = 1e-06
routed_scale = 2.5

def reference(tokens, expert_ids, affinity, norm_gain, gate_train, up_train, down_train, shared_gate_train, shared_up_train, shared_down_train):
    gain_cols = norm_gain[None, None, :]
    gate_serve = (gate_train * gain_cols).astype(jnp.bfloat16)
    up_serve = (up_train * gain_cols).astype(jnp.bfloat16)
    down_serve = down_train.astype(jnp.bfloat16)
    shared_gate_serve = (shared_gate_train * norm_gain[None, :]).astype(jnp.bfloat16)
    shared_up_serve = (shared_up_train * norm_gain[None, :]).astype(jnp.bfloat16)
    shared_down_serve = shared_down_train.astype(jnp.bfloat16)
    widened = tokens.astype(jnp.float32)
    inverse_rms = lax.rsqrt(lax.optimization_barrier(jnp.mean(widened * widened, axis=1)) + norm_eps)
    shared_gate = jnp.dot(tokens, shared_gate_serve.T, preferred_element_type=jnp.float32) * inverse_rms[:, None]
    shared_up = jnp.dot(tokens, shared_up_serve.T, preferred_element_type=jnp.float32) * inverse_rms[:, None]
    shared_hidden = (jax.nn.silu(shared_gate) * shared_up).astype(jnp.bfloat16)
    shared_out = jnp.dot(shared_hidden, shared_down_serve, preferred_element_type=jnp.float32)
    ids = expert_ids.reshape(N_FS, TOK * K)
    onehot = (ids[:, :, None] == jnp.arange(EXPERTS, dtype=jnp.int32)[None, None, :]).astype(jnp.int32)
    slot_index = lax.optimization_barrier(jnp.sum((jnp.cumsum(onehot, axis=1) - onehot) * onehot, axis=2))
    block_index = jnp.arange(N_FS, dtype=jnp.int32)[:, None]
    position = (ids * (N_FS * CAP) + block_index * CAP + slot_index).reshape(-1).astype(jnp.int32)
    token_of = jnp.repeat(jnp.arange(TOKENS, dtype=jnp.int32), K)
    rows = jnp.zeros((EXPERTS * N_FS * CAP, D), jnp.bfloat16).at[position].set(tokens[token_of])
    scales = jnp.zeros((EXPERTS * N_FS * CAP,), jnp.float32).at[position].set(inverse_rms[token_of])

    def one_expert(operands):
        rows_e, scale_e, gate_w, up_w, down_w = operands
        gate_pre = jnp.dot(rows_e, gate_w.T, preferred_element_type=jnp.float32) * scale_e[:, None]
        up_pre = jnp.dot(rows_e, up_w.T, preferred_element_type=jnp.float32) * scale_e[:, None]
        hidden = (jax.nn.silu(gate_pre) * up_pre).astype(jnp.bfloat16)
        return jnp.dot(hidden, down_w, preferred_element_type=jnp.float32).astype(jnp.bfloat16)
    outputs = lax.map(one_expert, (rows.reshape(EXPERTS, N_FS * CAP, D), scales.reshape(EXPERTS, N_FS * CAP), gate_serve, up_serve, down_serve))
    picked = outputs.reshape(EXPERTS * N_FS * CAP, D)[position].reshape(TOKENS, K, D).astype(jnp.float32)
    route_weight = routed_scale * affinity / lax.optimization_barrier(jnp.sum(affinity, axis=1, keepdims=True))
    routed = lax.optimization_barrier(jnp.sum(picked * route_weight[:, :, None], axis=1))
    mixed = (shared_out + routed).astype(jnp.bfloat16)
    return (mixed, gate_serve, up_serve, down_serve, shared_gate_serve, shared_up_serve, shared_down_serve)
```

```python
import functools

import jax
import jax.numpy as jnp
from jax import lax
from jax.experimental import pallas as pl
from jax.experimental.pallas import tpu as pltpu
from jax.sharding import PartitionSpec as P

MESH = pl.DeviceIdType.MESH

norm_eps = 1e-06
routed_scale = 2.5


def exchange_kernel(n, specs, nsmall, *refs):
    nw = len(specs)
    nbig = nw - nsmall
    ins = refs[:nw]
    gain_ref = refs[nw]
    outs = refs[nw + 1 : 2 * nw + 1]
    scr = list(refs[2 * nw + 1 :])
    fbuf, lsem, ssem, rsem, osem = scr[:5]
    bufs = scr[5:]
    me = lax.axis_index("fs")
    dest = [lax.rem(me + k, n) for k in range(n)]

    barrier = pltpu.get_barrier_semaphore()
    for k in range(1, n):
        pl.semaphore_signal(barrier, inc=1, device_id={"fs": dest[k]}, device_id_type=MESH)
    pl.semaphore_wait(barrier, n - 1)

    def place(w, who, first, count):
        cut, _ = specs[w]
        width = ins[w].shape[cut]
        part = pl.ds(pl.multiple_of(who * width, width), width)
        if w >= nbig:
            return outs[w].at[part, :] if cut == 0 else outs[w].at[:, part]
        if cut == 1:
            return outs[w].at[pl.ds(first, count), part, :]
        return outs[w].at[pl.ds(first, count), :, part]

    def remote(w, k, src, first, count):
        return pltpu.make_async_remote_copy(
            src_ref=src,
            dst_ref=place(w, me, first, count),
            send_sem=ssem.at[w, k],
            recv_sem=rsem.at[w, k],
            device_id={"fs": dest[k]},
            device_id_type=MESH,
        )

    small = range(nbig, nw)
    for w in small:
        pltpu.make_async_copy(ins[w], bufs[nw + w - nbig], osem.at[w]).start()
    order = list(range(1, n)) + [0]
    for w in range(nbig):
        cut, scaled = specs[w]
        local = outs[w].shape[0]
        chunk = fbuf.shape[1]
        shape = ins[w].shape[1:]
        steps = local // chunk
        view = fbuf if fbuf.shape[2:] == shape else None
        assert view is not None

        def load(j, k, w=w, local=local, chunk=chunk):
            return pltpu.make_async_copy(
                ins[w].at[pl.ds(dest[k] * local + j * chunk, chunk)], fbuf.at[k], lsem.at[k]
            )

        for k in order:
            load(0, k).start()
        if w == 0:
            for s in small:
                pltpu.make_async_copy(ins[s], bufs[nw + s - nbig], osem.at[s]).wait()
                value = bufs[nw + s - nbig][...]
                if specs[s][1]:
                    value = value * gain_ref[...]
                bufs[s][...] = value.astype(jnp.bfloat16)

        def step(j, carry, w=w, chunk=chunk, steps=steps, scaled=scaled, load=load):
            first = j * chunk
            pending = None
            for k in order:
                load(j, k).wait()
                for c in range(chunk):
                    value = fbuf[k, c]
                    if scaled:
                        value = value * gain_ref[...]
                    bufs[w][k, first + c] = value.astype(jnp.bfloat16)

                @pl.when(j + 1 < steps)
                def _():
                    load(j + 1, k).start()

                if pending is not None:
                    remote(w, pending, bufs[w].at[pending, pl.ds(first, chunk)], first, chunk).start()
                pending = k
            pltpu.make_async_copy(
                bufs[w].at[0, pl.ds(first, chunk)], place(w, me, first, chunk), osem.at[w]
            ).start()
            return carry

        lax.fori_loop(0, steps, step, 0)
    for s in small:
        for k in order[:-1]:
            remote(s, k, bufs[s], 0, 0).start()
        pltpu.make_async_copy(bufs[s], place(s, me, 0, 0), osem.at[s]).start()

    for w in range(nw):
        big = w < nbig
        local = outs[w].shape[0] if big else 0
        for k in range(1, n):
            src = bufs[w].at[k] if big else bufs[w]
            source = lax.rem(me + n - k, n)
            pltpu.make_async_remote_copy(
                src_ref=src,
                dst_ref=place(w, source, 0, local),
                send_sem=ssem.at[w, k],
                recv_sem=rsem.at[w, k],
                device_id={"fs": dest[k]},
                device_id_type=MESH,
            ).wait()
        own = bufs[w].at[0] if big else bufs[w]
        pltpu.make_async_copy(own, place(w, me, 0, local), osem.at[w]).wait()


def exchange(n, weights, smalls, gain, collective_id):
    both = weights + smalls
    outs, bufs = [], []
    for a, cut, _ in weights:
        dims = list(a.shape)
        dims[0] //= n
        bufs.append(pltpu.VMEM((n, *dims), jnp.bfloat16))
        dims[cut] *= n
        outs.append(jax.ShapeDtypeStruct(tuple(dims), jnp.bfloat16))
    for a, cut, _ in smalls:
        dims = list(a.shape)
        bufs.append(pltpu.VMEM(tuple(dims), jnp.bfloat16))
        dims[cut] *= n
        outs.append(jax.ShapeDtypeStruct(tuple(dims), jnp.bfloat16))
    for a, _, _ in smalls:
        bufs.append(pltpu.VMEM(a.shape, jnp.float32))
    local = weights[0][0].shape[0] // n
    chunk = 2 if local % 2 == 0 else 1
    sent = sum(2 * a.size * (n - 1) // n for a, _, _ in weights)
    nw = len(both)
    any_spec = pl.BlockSpec(memory_space=pl.ANY)
    return pl.pallas_call(
        functools.partial(exchange_kernel, n, [(c, g) for _, c, g in both], len(smalls)),
        out_shape=tuple(outs),
        in_specs=[any_spec] * nw + [pl.BlockSpec(memory_space=pltpu.VMEM)],
        out_specs=(any_spec,) * nw,
        scratch_shapes=[
            pltpu.VMEM((n, chunk, *weights[0][0].shape[1:]), jnp.float32),
            pltpu.SemaphoreType.DMA((n,)),
            pltpu.SemaphoreType.DMA((nw, n)),
            pltpu.SemaphoreType.DMA((nw, n)),
            pltpu.SemaphoreType.DMA((nw,)),
            *bufs,
        ],
        compiler_params=pltpu.CompilerParams(
            collective_id=collective_id, has_side_effects=True, vmem_limit_bytes=48 * 2**20
        ),
        cost_estimate=pl.CostEstimate(flops=0, bytes_accessed=40 * sent, transcendentals=0),
    )(*[a for a, _, _ in both], gain)


def nt_dot(a, b):
    return lax.dot_general(a, b, (((1,), (1,)), ((), ())), preferred_element_type=jnp.float32)


def up_kernel(
    own_rows, pairs, x_ref, route_ref, g_ref, u_ref, sg_ref, su_ref, hid_ref, go_ref, uo_ref, sgo_ref, suo_ref, inv_ref
):
    p = pl.program_id(0)
    parts, rows, width = x_ref.shape
    d = parts * width
    topk = route_ref.shape[1] // 2
    me = lax.axis_index("fs")

    @pl.when(p == 0)
    def _():
        total = jnp.zeros((rows, 1), jnp.float32)
        for i in range(parts):
            x = x_ref[i].astype(jnp.float32)
            total = total + jnp.sum(x * x, axis=1, keepdims=True)
        inv_ref[...] = jnp.broadcast_to(lax.rsqrt(total / d + norm_eps), inv_ref.shape)
        sgo_ref[...] = sg_ref[...]
        suo_ref[...] = su_ref[...]

    def hidden(g, u):
        acc = None
        for i in range(parts):
            cols = slice(i * width, (i + 1) * width)
            both = jnp.concatenate([g[:, cols], u[:, cols]], axis=0)
            term = nt_dot(x_ref[i], both)
            acc = term if acc is None else acc + term
        half = acc.shape[1] // 2
        gate = acc[:, :half] * inv_ref[:, :1]
        up = acc[:, half:] * inv_ref[:, :1]
        return gate / (1.0 + jnp.exp(-gate)) * up

    @pl.when(p < pairs)
    def _():
        g, u = g_ref[...], u_ref[...]
        go_ref[...] = g
        uo_ref[...] = u
        h = hidden(g.reshape(-1, d), u.reshape(-1, d))
        per = h.shape[1] // 2
        lane = lax.broadcasted_iota(jnp.int32, h.shape, 1)
        expert = (me * (2 * pairs) + 2 * p + jnp.where(lane >= per, 1, 0)).astype(jnp.float32)
        weight = jnp.zeros(h.shape, jnp.float32)
        for k in range(topk):
            weight = weight + jnp.where(
                route_ref[:, k : k + 1] == expert, route_ref[:, topk + k : topk + k + 1], 0.0
            )
        hid_ref[...] = (h * weight).astype(jnp.bfloat16)[None]

    @pl.when(p == pairs)
    def _():
        h = hidden(sg_ref[...], su_ref[...])
        row = lax.broadcasted_iota(jnp.int32, h.shape, 0)
        mine = (row >= me * own_rows) & (row < (me + 1) * own_rows)
        h = jnp.where(mine, h, 0.0).astype(jnp.bfloat16)
        hid_ref[...] = jnp.concatenate([h, jnp.zeros_like(h)], axis=1)[None]


def up_call(own_rows, x, route, gate, up, sg, su):
    experts, hl, d = gate.shape
    pairs = experts // 2
    parts, rows, width = x.shape
    whole = pl.BlockSpec(memory_space=pltpu.VMEM)
    pair_spec = pl.BlockSpec((2, hl, d), lambda p: (jnp.minimum(p, pairs - 1), 0, 0))
    return pl.pallas_call(
        functools.partial(up_kernel, own_rows, pairs),
        grid=(pairs + 1,),
        out_shape=(
            jax.ShapeDtypeStruct((pairs + 1, rows, 2 * hl), jnp.bfloat16),
            jax.ShapeDtypeStruct(gate.shape, gate.dtype),
            jax.ShapeDtypeStruct(up.shape, up.dtype),
            jax.ShapeDtypeStruct(sg.shape, sg.dtype),
            jax.ShapeDtypeStruct(su.shape, su.dtype),
        ),
        in_specs=[whole, whole, pair_spec, pair_spec, whole, whole],
        out_specs=(
            pl.BlockSpec((1, rows, 2 * hl), lambda p: (p, 0, 0)),
            pair_spec,
            pair_spec,
            whole,
            whole,
        ),
        scratch_shapes=[pltpu.VMEM((rows, 128), jnp.float32)],
        compiler_params=pltpu.CompilerParams(vmem_limit_bytes=56 * 2**20),
        cost_estimate=pl.CostEstimate(
            flops=4 * rows * d * hl * (experts + 1), bytes_accessed=8 * gate.size, transcendentals=0
        ),
    )(x, route, gate, up, sg, su)


def down_kernel(hid_ref, d_ref, sd_ref, out_ref, do_ref, sdo_ref, acc_ref):
    i = pl.program_id(0)
    d = d_ref[...]
    do_ref[...] = d
    sd = sd_ref[...]
    sdo_ref[...] = sd
    pairs = hid_ref.shape[1] - 1
    hl = sd.shape[0]
    total = jnp.dot(
        hid_ref[0, pairs][:, :hl], sd, preferred_element_type=jnp.float32
    )
    for p in range(pairs):
        total = total + jnp.dot(
            hid_ref[0, p], d[2 * p : 2 * p + 2].reshape(2 * hl, -1), preferred_element_type=jnp.float32
        )

    @pl.when(i == 0)
    def _():
        acc_ref[...] = total

    @pl.when(i > 0)
    def _():
        acc_ref[...] += total

    @pl.when(i == pl.num_programs(0) - 1)
    def _():
        out_ref[...] = acc_ref[...].astype(jnp.bfloat16)


def down_call(hid, down, sd):
    parts, blocks, rows, _ = hid.shape
    experts, h, d = down.shape
    hl = h // parts
    d_spec = pl.BlockSpec((experts, hl, d), lambda i: (0, i, 0))
    sd_spec = pl.BlockSpec((hl, d), lambda i: (i, 0))
    return pl.pallas_call(
        down_kernel,
        grid=(parts,),
        out_shape=(
            jax.ShapeDtypeStruct((rows, d), jnp.bfloat16),
            jax.ShapeDtypeStruct(down.shape, down.dtype),
            jax.ShapeDtypeStruct(sd.shape, sd.dtype),
        ),
        in_specs=[pl.BlockSpec((1, blocks, rows, hid.shape[3]), lambda i: (i, 0, 0, 0)), d_spec, sd_spec],
        out_specs=(pl.BlockSpec((rows, d), lambda i: (0, 0)), d_spec, sd_spec),
        scratch_shapes=[pltpu.VMEM((rows, d), jnp.float32)],
        compiler_params=pltpu.CompilerParams(vmem_limit_bytes=48 * 2**20),
        cost_estimate=pl.CostEstimate(flops=2 * rows * d * experts * h, bytes_accessed=6 * down.size, transcendentals=0),
    )(hid, down, sd)


def body(
    n,
    tokens,
    expert_ids,
    affinity,
    norm_gain,
    gate_train,
    up_train,
    down_train,
    shared_gate_train,
    shared_up_train,
    shared_down_train,
):
    own_rows = tokens.shape[0]
    route_weight = routed_scale * affinity / jnp.sum(affinity, axis=1, keepdims=True)
    route = jnp.concatenate([expert_ids.astype(jnp.float32), route_weight], axis=1)
    route = lax.all_gather(route, "fs", axis=0, tiled=True)
    columns = lax.all_gather(tokens, "fs", axis=0, tiled=True)
    gain, columns, route = lax.optimization_barrier((norm_gain[None, :], columns, route))
    x = lax.all_gather(columns, "tp", axis=0)
    gate, up, sg, su, sd = exchange(
        n,
        [(gate_train, 2, True), (up_train, 2, True)],
        [(shared_gate_train, 1, True), (shared_up_train, 1, True), (shared_down_train, 0, False)],
        gain,
        0,
    )
    hid, gate_serve, up_serve, shared_gate_serve, shared_up_serve = up_call(own_rows, x, route, gate, up, sg, su)
    down_in, hid = lax.optimization_barrier((down_train, hid))
    every = lax.all_gather(hid, "tp", axis=0)
    (down,) = exchange(n, [(down_in, 1, False)], [], gain, 1)
    part, down_serve, shared_down_serve = down_call(every, down, sd)
    part = lax.all_to_all(part.reshape(n, own_rows, -1), "fs", split_axis=0, concat_axis=0, tiled=True)
    mixed = jnp.sum(part.astype(jnp.float32), axis=0).astype(jnp.bfloat16)
    return (
        mixed,
        gate_serve,
        up_serve,
        down_serve,
        shared_gate_serve,
        shared_up_serve,
        shared_down_serve,
    )


def solution(mesh):
    return jax.shard_map(
        functools.partial(body, mesh.shape["fs"]),
        mesh=mesh,
        in_specs=(
            P("fs", "tp"),
            P("fs", None),
            P("fs", None),
            P("fs"),
            P(None, "tp", "fs"),
            P(None, "tp", "fs"),
            P(None, "fs", "tp"),
            P("tp", "fs"),
            P("tp", "fs"),
            P("fs", "tp"),
        ),
        out_specs=(
            P("fs", "tp"),
            P("fs", "tp", None),
            P("fs", "tp", None),
            P("fs", None, "tp"),
            P("tp", None),
            P("tp", None),
            P(None, "tp"),
        ),
        check_vma=False,
    )
```

```python
import functools

import jax
import jax.numpy as jnp
from jax import lax
from jax.experimental import pallas as pl
from jax.experimental.pallas import tpu as pltpu
from jax.sharding import PartitionSpec as P

MESH = pl.DeviceIdType.MESH

norm_eps = 1e-06
routed_scale = 2.5


def exchange_kernel(n, ntp, specs, nsmall, *refs):
    nw = len(specs)
    nbig = nw - nsmall
    extra = 2 if ntp else 0
    ins = refs[:nw]
    gain_ref = refs[nw]
    refs = refs[nw + 1 :]
    if ntp:
        tok_ref, route_ref = refs[:2]
    outs = refs[extra : extra + nw]
    if ntp:
        x_ref, routes_ref = refs[extra + nw : 2 * extra + nw]
    scr = list(refs[2 * extra + nw :])
    fbuf, lsem, ssem, rsem, osem = scr[:5]
    bufs = scr[5:]
    me = lax.axis_index("fs")
    dest = [lax.rem(me + k, n) for k in range(n)]
    if ntp:
        cols, tsem, zsem, zrsem, zosem = scr[-5:]
        tp = lax.axis_index("tp")
        tdest = [lax.rem(tp + k, ntp) for k in range(ntp)]

    barrier = pltpu.get_barrier_semaphore()
    for k in range(1, n):
        pl.semaphore_signal(barrier, inc=1, device_id={"fs": dest[k]}, device_id_type=MESH)
    for k in range(1, ntp):
        pl.semaphore_signal(barrier, inc=1, device_id={"tp": tdest[k]}, device_id_type=MESH)
    pl.semaphore_wait(barrier, n - 1 + max(ntp - 1, 0))

    def token_copy(k, source):
        rows = tok_ref.shape[0]
        return pltpu.make_async_remote_copy(
            src_ref=tok_ref,
            dst_ref=cols.at[pl.ds(pl.multiple_of(source * rows, rows), rows)],
            send_sem=tsem.at[0, k],
            recv_sem=tsem.at[1, k],
            device_id={"fs": dest[k]},
            device_id_type=MESH,
        )

    def route_copy(k, source):
        rows = route_ref.shape[0]
        return pltpu.make_async_remote_copy(
            src_ref=route_ref,
            dst_ref=routes_ref.at[pl.ds(pl.multiple_of(source * rows, rows), rows)],
            send_sem=tsem.at[2, k],
            recv_sem=tsem.at[3, k],
            device_id={"fs": dest[k]},
            device_id_type=MESH,
        )

    def own_token_copy():
        rows = tok_ref.shape[0]
        return pltpu.make_async_copy(
            tok_ref, cols.at[pl.ds(pl.multiple_of(me * rows, rows), rows)], tsem.at[0, 0]
        )

    def own_route_copy():
        rows = route_ref.shape[0]
        return pltpu.make_async_copy(
            route_ref, routes_ref.at[pl.ds(pl.multiple_of(me * rows, rows), rows)], tsem.at[2, 0]
        )

    def column_part(source):
        width = cols.shape[1]
        return x_ref.at[:, pl.ds(pl.multiple_of(source * width, width), width)]

    def column_copy(k, source):
        return pltpu.make_async_remote_copy(
            src_ref=cols,
            dst_ref=column_part(source),
            send_sem=zsem.at[k],
            recv_sem=zrsem.at[k],
            device_id={"tp": tdest[k]},
            device_id_type=MESH,
        )

    if ntp:
        for k in range(1, n):
            token_copy(k, me).start()
            route_copy(k, me).start()
        own_token_copy().start()
        own_route_copy().start()

    def place(w, who, first, count):
        cut, _ = specs[w]
        width = ins[w].shape[cut]
        part = pl.ds(pl.multiple_of(who * width, width), width)
        if w >= nbig:
            return outs[w].at[part, :] if cut == 0 else outs[w].at[:, part]
        if cut == 1:
            return outs[w].at[pl.ds(first, count), part, :]
        return outs[w].at[pl.ds(first, count), :, part]

    def remote(w, k, src, first, count):
        return pltpu.make_async_remote_copy(
            src_ref=src,
            dst_ref=place(w, me, first, count),
            send_sem=ssem.at[w, k],
            recv_sem=rsem.at[w, k],
            device_id={"fs": dest[k]},
            device_id_type=MESH,
        )

    small = range(nbig, nw)
    for w in small:
        pltpu.make_async_copy(ins[w], bufs[nw + w - nbig], osem.at[w]).start()
    order = list(range(1, n)) + [0]
    for w in range(nbig):
        cut, scaled = specs[w]
        local = outs[w].shape[0]
        chunk = fbuf.shape[1]
        shape = ins[w].shape[1:]
        steps = local // chunk
        view = fbuf if fbuf.shape[2:] == shape else None
        assert view is not None

        def load(j, k, w=w, local=local, chunk=chunk):
            return pltpu.make_async_copy(
                ins[w].at[pl.ds(dest[k] * local + j * chunk, chunk)], fbuf.at[k], lsem.at[k]
            )

        for k in order:
            load(0, k).start()
        if w == 0:
            for s in small:
                pltpu.make_async_copy(ins[s], bufs[nw + s - nbig], osem.at[s]).wait()
                value = bufs[nw + s - nbig][...]
                if specs[s][1]:
                    value = value * gain_ref[...]
                bufs[s][...] = value.astype(jnp.bfloat16)

        def step(j, carry, w=w, chunk=chunk, steps=steps, scaled=scaled, load=load):
            first = j * chunk
            pending = None
            for k in order:
                load(j, k).wait()
                for c in range(chunk):
                    value = fbuf[k, c]
                    if scaled:
                        value = value * gain_ref[...]
                    bufs[w][k, first + c] = value.astype(jnp.bfloat16)

                @pl.when(j + 1 < steps)
                def _():
                    load(j + 1, k).start()

                if pending is not None:
                    remote(w, pending, bufs[w].at[pending, pl.ds(first, chunk)], first, chunk).start()
                pending = k
            pltpu.make_async_copy(
                bufs[w].at[0, pl.ds(first, chunk)], place(w, me, first, chunk), osem.at[w]
            ).start()
            return carry

        lax.fori_loop(0, steps, step, 0)
        if ntp and w == 0:
            for k in range(1, n):
                token_copy(k, lax.rem(me + n - k, n)).wait()
            own_token_copy().wait()
            for k in range(1, ntp):
                column_copy(k, tp).start()
            pltpu.make_async_copy(cols, column_part(tp), zosem).start()
    for s in small:
        for k in order[:-1]:
            remote(s, k, bufs[s], 0, 0).start()
        pltpu.make_async_copy(bufs[s], place(s, me, 0, 0), osem.at[s]).start()

    for w in range(nw):
        big = w < nbig
        local = outs[w].shape[0] if big else 0
        for k in range(1, n):
            src = bufs[w].at[k] if big else bufs[w]
            source = lax.rem(me + n - k, n)
            pltpu.make_async_remote_copy(
                src_ref=src,
                dst_ref=place(w, source, 0, local),
                send_sem=ssem.at[w, k],
                recv_sem=rsem.at[w, k],
                device_id={"fs": dest[k]},
                device_id_type=MESH,
            ).wait()
        own = bufs[w].at[0] if big else bufs[w]
        pltpu.make_async_copy(own, place(w, me, 0, local), osem.at[w]).wait()
    if ntp:
        for k in range(1, n):
            route_copy(k, lax.rem(me + n - k, n)).wait()
        own_route_copy().wait()
        for k in range(1, ntp):
            column_copy(k, lax.rem(tp + ntp - k, ntp)).wait()
        pltpu.make_async_copy(cols, column_part(tp), zosem).wait()


def exchange(n, ntp, weights, smalls, gain, tokens, collective_id):
    both = weights + smalls
    outs, bufs = [], []
    for a, cut, _ in weights:
        dims = list(a.shape)
        dims[0] //= n
        bufs.append(pltpu.VMEM((n, *dims), jnp.bfloat16))
        dims[cut] *= n
        outs.append(jax.ShapeDtypeStruct(tuple(dims), jnp.bfloat16))
    for a, cut, _ in smalls:
        dims = list(a.shape)
        bufs.append(pltpu.VMEM(tuple(dims), jnp.bfloat16))
        dims[cut] *= n
        outs.append(jax.ShapeDtypeStruct(tuple(dims), jnp.bfloat16))
    for a, _, _ in smalls:
        bufs.append(pltpu.VMEM(a.shape, jnp.float32))
    local = weights[0][0].shape[0] // n
    chunk = 2 if local % 2 == 0 else 1
    sent = sum(2 * a.size * (n - 1) // n for a, _, _ in weights)
    nw = len(both)
    any_spec = pl.BlockSpec(memory_space=pltpu.HBM)
    more, sems = [], []
    if ntp:
        (t, cols), (r, lanes) = tokens[0].shape, tokens[1].shape
        outs += [
            jax.ShapeDtypeStruct((n * t, ntp * cols), jnp.bfloat16),
            jax.ShapeDtypeStruct((n * r, lanes), jnp.float32),
        ]
        sems = [
            pltpu.VMEM((n * t, cols), jnp.bfloat16),
            pltpu.SemaphoreType.DMA((4, n)),
            pltpu.SemaphoreType.DMA((ntp,)),
            pltpu.SemaphoreType.DMA((ntp,)),
            pltpu.SemaphoreType.DMA,
        ]
        more = list(tokens)
    return pl.pallas_call(
        functools.partial(exchange_kernel, n, ntp, [(c, g) for _, c, g in both], len(smalls)),
        out_shape=tuple(outs),
        in_specs=[any_spec] * nw + [pl.BlockSpec(memory_space=pltpu.VMEM)] + [any_spec] * len(more),
        out_specs=(any_spec,) * (nw + len(more)),
        scratch_shapes=[
            pltpu.VMEM((n, chunk, *weights[0][0].shape[1:]), jnp.float32),
            pltpu.SemaphoreType.DMA((n,)),
            pltpu.SemaphoreType.DMA((nw, n)),
            pltpu.SemaphoreType.DMA((nw, n)),
            pltpu.SemaphoreType.DMA((nw,)),
            *bufs,
            *sems,
        ],
        compiler_params=pltpu.CompilerParams(
            collective_id=collective_id, has_side_effects=True, vmem_limit_bytes=48 * 2**20
        ),
        cost_estimate=pl.CostEstimate(flops=0, bytes_accessed=40 * sent, transcendentals=0),
    )(*[a for a, _, _ in both], gain, *more)


def nt_dot(a, b):
    return lax.dot_general(a, b, (((1,), (1,)), ((), ())), preferred_element_type=jnp.float32)


def up_kernel(
    own_rows, pairs, group, x_ref, route_ref, g_ref, u_ref, sg_ref, su_ref, hid_ref, go_ref, uo_ref, sgo_ref, suo_ref, inv_ref
):
    p = pl.program_id(0)
    rows, d = x_ref.shape
    topk = route_ref.shape[1] // 2
    me = lax.axis_index("fs")

    @pl.when(p == 0)
    def _():
        total = jnp.zeros((rows, 1), jnp.float32)
        width = 512
        for i in range(0, d, width):
            x = x_ref[:, i : i + width].astype(jnp.float32)
            total = total + jnp.sum(x * x, axis=1, keepdims=True)
        inv_ref[...] = jnp.broadcast_to(lax.rsqrt(total / d + norm_eps), inv_ref.shape)
        sgo_ref[...] = sg_ref[...]
        suo_ref[...] = su_ref[...]

    def hidden(g, u):
        acc = nt_dot(x_ref[...], jnp.concatenate([g, u], axis=0))
        half = acc.shape[1] // 2
        gate = acc[:, :half] * inv_ref[:, :1]
        up = acc[:, half:] * inv_ref[:, :1]
        return gate / (1.0 + jnp.exp(-gate)) * up

    @pl.when(p < pairs)
    def _():
        g, u = g_ref[...], u_ref[...]
        go_ref[...] = g
        uo_ref[...] = u
        h = hidden(g.reshape(-1, d), u.reshape(-1, d))
        per = h.shape[1] // group
        lane = lax.broadcasted_iota(jnp.int32, h.shape, 1)
        expert = (me * (group * pairs) + group * p + lane // per).astype(jnp.float32)
        weight = jnp.zeros(h.shape, jnp.float32)
        for k in range(topk):
            weight = weight + jnp.where(
                route_ref[:, k : k + 1] == expert, route_ref[:, topk + k : topk + k + 1], 0.0
            )
        hid_ref[...] = (h * weight).astype(jnp.bfloat16)

    @pl.when(p == pairs)
    def _():
        h = hidden(sg_ref[...], su_ref[...])
        row = lax.broadcasted_iota(jnp.int32, h.shape, 0)
        mine = (row >= me * own_rows) & (row < (me + 1) * own_rows)
        h = jnp.where(mine, h, 0.0).astype(jnp.bfloat16)
        hid_ref[...] = jnp.concatenate([h] + [jnp.zeros_like(h)] * (group - 1), axis=1)


def up_call(own_rows, x, route, gate, up, sg, su):
    experts, hl, d = gate.shape
    group = min(experts, max(1, 128 // hl))
    pairs = experts // group
    rows = x.shape[0]
    whole = pl.BlockSpec(memory_space=pltpu.VMEM)
    pair_spec = pl.BlockSpec((group, hl, d), lambda p: (jnp.minimum(p, pairs - 1), 0, 0))
    return pl.pallas_call(
        functools.partial(up_kernel, own_rows, pairs, group),
        grid=(pairs + 1,),
        out_shape=(
            jax.ShapeDtypeStruct((rows, (pairs + 1) * group * hl), jnp.bfloat16),
            jax.ShapeDtypeStruct(gate.shape, gate.dtype),
            jax.ShapeDtypeStruct(up.shape, up.dtype),
            jax.ShapeDtypeStruct(sg.shape, sg.dtype),
            jax.ShapeDtypeStruct(su.shape, su.dtype),
        ),
        in_specs=[whole, whole, pair_spec, pair_spec, whole, whole],
        out_specs=(
            pl.BlockSpec((rows, group * hl), lambda p: (0, p)),
            pair_spec,
            pair_spec,
            whole,
            whole,
        ),
        scratch_shapes=[pltpu.VMEM((rows, 128), jnp.float32)],
        compiler_params=pltpu.CompilerParams(vmem_limit_bytes=56 * 2**20),
        cost_estimate=pl.CostEstimate(
            flops=4 * rows * d * hl * (experts + 1), bytes_accessed=8 * gate.size, transcendentals=0
        ),
    )(x, route, gate, up, sg, su)


def down_kernel(hid_ref, d_ref, sd_ref, out_ref, do_ref, sdo_ref, acc_ref):
    i = pl.program_id(0)
    d = d_ref[...]
    do_ref[...] = d
    sd = sd_ref[...]
    sdo_ref[...] = sd
    hl = sd.shape[0]
    wide = d.shape[0] * hl
    total = jnp.dot(hid_ref[0, :, :wide], d.reshape(wide, -1), preferred_element_type=jnp.float32)
    total += jnp.dot(hid_ref[0, :, wide : wide + hl], sd, preferred_element_type=jnp.float32)

    @pl.when(i == 0)
    def _():
        acc_ref[...] = total

    @pl.when(i > 0)
    def _():
        acc_ref[...] += total

    @pl.when(i == pl.num_programs(0) - 1)
    def _():
        out_ref[...] = acc_ref[...].astype(jnp.bfloat16)


def down_call(hid, down, sd):
    parts, rows, lanes = hid.shape
    experts, h, d = down.shape
    hl = h // parts
    d_spec = pl.BlockSpec((experts, hl, d), lambda i: (0, i, 0))
    sd_spec = pl.BlockSpec((hl, d), lambda i: (i, 0))
    return pl.pallas_call(
        down_kernel,
        grid=(parts,),
        out_shape=(
            jax.ShapeDtypeStruct((rows, d), jnp.bfloat16),
            jax.ShapeDtypeStruct(down.shape, down.dtype),
            jax.ShapeDtypeStruct(sd.shape, sd.dtype),
        ),
        in_specs=[pl.BlockSpec((1, rows, lanes), lambda i: (i, 0, 0)), d_spec, sd_spec],
        out_specs=(pl.BlockSpec((rows, d), lambda i: (0, 0)), d_spec, sd_spec),
        scratch_shapes=[pltpu.VMEM((rows, d), jnp.float32)],
        compiler_params=pltpu.CompilerParams(vmem_limit_bytes=48 * 2**20),
        cost_estimate=pl.CostEstimate(flops=2 * rows * d * experts * h, bytes_accessed=6 * down.size, transcendentals=0),
    )(hid, down, sd)


def combine_kernel(n, part_ref, out_ref, landed, ssem, rsem):
    me = lax.axis_index("fs")
    rows = out_ref.shape[0]
    barrier = pltpu.get_barrier_semaphore()
    for k in range(1, n):
        pl.semaphore_signal(barrier, inc=1, device_id={"fs": lax.rem(me + k, n)}, device_id_type=MESH)
    pl.semaphore_wait(barrier, n - 1)

    def block(who):
        return part_ref.at[pl.ds(pl.multiple_of(who * rows, rows), rows)]

    copies = []
    for k in range(1, n):
        to = lax.rem(me + k, n)
        copy = pltpu.make_async_remote_copy(
            src_ref=block(to),
            dst_ref=landed.at[k - 1],
            send_sem=ssem.at[k - 1],
            recv_sem=rsem.at[k - 1],
            device_id={"fs": to},
            device_id_type=MESH,
        )
        copy.start()
        copies.append(copy)
    total = block(me)[...].astype(jnp.float32)
    for k in range(1, n):
        copies[k - 1].wait()
        total = total + landed[k - 1].astype(jnp.float32)
    out_ref[...] = total.astype(out_ref.dtype)


def combine(n, part, collective_id):
    rows, d = part.shape[0] // n, part.shape[1]
    vmem = pl.BlockSpec(memory_space=pltpu.VMEM)
    return pl.pallas_call(
        functools.partial(combine_kernel, n),
        out_shape=jax.ShapeDtypeStruct((rows, d), part.dtype),
        in_specs=[vmem],
        out_specs=vmem,
        scratch_shapes=[
            pltpu.VMEM((n - 1, rows, d), part.dtype),
            pltpu.SemaphoreType.DMA((n - 1,)),
            pltpu.SemaphoreType.DMA((n - 1,)),
        ],
        compiler_params=pltpu.CompilerParams(collective_id=collective_id, has_side_effects=True),
    )(part)


def body(
    n,
    ntp,
    tokens,
    expert_ids,
    affinity,
    norm_gain,
    gate_train,
    up_train,
    down_train,
    shared_gate_train,
    shared_up_train,
    shared_down_train,
):
    own_rows = tokens.shape[0]
    route_weight = routed_scale * affinity / jnp.sum(affinity, axis=1, keepdims=True)
    route = jnp.concatenate([expert_ids.astype(jnp.float32), route_weight], axis=1)
    gain = norm_gain[None, :]
    gate, up, sg, su, sd, x, route = exchange(
        n,
        ntp,
        [(gate_train, 2, True), (up_train, 2, True)],
        [(shared_gate_train, 1, True), (shared_up_train, 1, True), (shared_down_train, 0, False)],
        gain,
        (tokens, route),
        0,
    )
    hid, gate_serve, up_serve, shared_gate_serve, shared_up_serve = up_call(own_rows, x, route, gate, up, sg, su)
    down_in, hid = lax.optimization_barrier((down_train, hid))
    every = lax.all_gather(hid, "tp", axis=0)
    (down,) = exchange(n, 0, [(down_in, 1, False)], [], gain, None, 1)
    part, down_serve, shared_down_serve = down_call(every, down, sd)
    mixed = combine(n, part, 2)
    return (
        mixed,
        gate_serve,
        up_serve,
        down_serve,
        shared_gate_serve,
        shared_up_serve,
        shared_down_serve,
    )


def solution(mesh):
    return jax.shard_map(
        functools.partial(body, mesh.shape["fs"], mesh.shape["tp"]),
        mesh=mesh,
        in_specs=(
            P("fs", "tp"),
            P("fs", None),
            P("fs", None),
            P("fs"),
            P(None, "tp", "fs"),
            P(None, "tp", "fs"),
            P(None, "fs", "tp"),
            P("tp", "fs"),
            P("tp", "fs"),
            P("fs", "tp"),
        ),
        out_specs=(
            P("fs", "tp"),
            P("fs", "tp", None),
            P("fs", "tp", None),
            P("fs", None, "tp"),
            P("tp", None),
            P("tp", None),
            P(None, "tp"),
        ),
        check_vma=False,
    )
```

```python
import functools

import jax
import jax.numpy as jnp
from jax import lax
from jax.experimental import pallas as pl
from jax.experimental.pallas import tpu as pltpu
from jax.sharding import PartitionSpec as P

MESH = pl.DeviceIdType.MESH

norm_eps = 1e-06
routed_scale = 2.5


def exchange_kernel(n, ntp, specs, nsmall, *refs):
    nw = len(specs)
    nbig = nw - nsmall
    extra = 2 if ntp else 0
    ins = refs[:nw]
    gain_ref = refs[nw]
    refs = refs[nw + 1 :]
    if ntp:
        tok_ref, route_ref = refs[:2]
    outs = refs[extra : extra + nw]
    if ntp:
        x_ref, routes_ref = refs[extra + nw : 2 * extra + nw]
    scr = list(refs[2 * extra + nw :])
    fbuf, lsem, ssem, rsem, osem = scr[:5]
    bufs = scr[5:]
    me = lax.axis_index("fs")
    dest = [lax.rem(me + k, n) for k in range(n)]
    if ntp:
        cols, tsem, zsem, zrsem, zosem = scr[-5:]
        tp = lax.axis_index("tp")
        tdest = [lax.rem(tp + k, ntp) for k in range(ntp)]

    barrier = pltpu.get_barrier_semaphore()
    for k in range(1, n):
        pl.semaphore_signal(barrier, inc=1, device_id={"fs": dest[k]}, device_id_type=MESH)
    for k in range(1, ntp):
        pl.semaphore_signal(barrier, inc=1, device_id={"tp": tdest[k]}, device_id_type=MESH)
    pl.semaphore_wait(barrier, n - 1 + max(ntp - 1, 0))

    def token_copy(k, source):
        rows = tok_ref.shape[0]
        return pltpu.make_async_remote_copy(
            src_ref=tok_ref,
            dst_ref=cols.at[pl.ds(pl.multiple_of(source * rows, rows), rows)],
            send_sem=tsem.at[0, k],
            recv_sem=tsem.at[1, k],
            device_id={"fs": dest[k]},
            device_id_type=MESH,
        )

    def route_copy(k, source):
        rows = route_ref.shape[0]
        return pltpu.make_async_remote_copy(
            src_ref=route_ref,
            dst_ref=routes_ref.at[pl.ds(pl.multiple_of(source * rows, rows), rows)],
            send_sem=tsem.at[2, k],
            recv_sem=tsem.at[3, k],
            device_id={"fs": dest[k]},
            device_id_type=MESH,
        )

    def own_token_copy():
        rows = tok_ref.shape[0]
        return pltpu.make_async_copy(
            tok_ref, cols.at[pl.ds(pl.multiple_of(me * rows, rows), rows)], tsem.at[0, 0]
        )

    def own_route_copy():
        rows = route_ref.shape[0]
        return pltpu.make_async_copy(
            route_ref, routes_ref.at[pl.ds(pl.multiple_of(me * rows, rows), rows)], tsem.at[2, 0]
        )

    def column_part(source):
        width = cols.shape[1]
        return x_ref.at[:, pl.ds(pl.multiple_of(source * width, width), width)]

    def column_copy(k, source):
        return pltpu.make_async_remote_copy(
            src_ref=cols,
            dst_ref=column_part(source),
            send_sem=zsem.at[k],
            recv_sem=zrsem.at[k],
            device_id={"tp": tdest[k]},
            device_id_type=MESH,
        )

    if ntp:
        for k in range(1, n):
            token_copy(k, me).start()
            route_copy(k, me).start()
        own_token_copy().start()
        own_route_copy().start()

    def place(w, who, first, count):
        cut, _ = specs[w]
        width = ins[w].shape[cut]
        part = pl.ds(pl.multiple_of(who * width, width), width)
        if w >= nbig:
            return outs[w].at[part, :] if cut == 0 else outs[w].at[:, part]
        if cut == 1:
            return outs[w].at[pl.ds(first, count), part, :]
        return outs[w].at[pl.ds(first, count), :, part]

    def remote(w, k, src, first, count):
        return pltpu.make_async_remote_copy(
            src_ref=src,
            dst_ref=place(w, me, first, count),
            send_sem=ssem.at[w, k],
            recv_sem=rsem.at[w, k],
            device_id={"fs": dest[k]},
            device_id_type=MESH,
        )

    small = range(nbig, nw)
    for w in small:
        pltpu.make_async_copy(ins[w], bufs[nw + w - nbig], osem.at[w]).start()
    order = list(range(1, n)) + [0]
    for w in range(nbig):
        cut, scaled = specs[w]
        local = outs[w].shape[0]
        chunk = fbuf.shape[1]
        shape = ins[w].shape[1:]
        steps = local // chunk
        view = fbuf if fbuf.shape[2:] == shape else None
        assert view is not None

        def load(j, k, w=w, local=local, chunk=chunk):
            return pltpu.make_async_copy(
                ins[w].at[pl.ds(dest[k] * local + j * chunk, chunk)], fbuf.at[k], lsem.at[k]
            )

        for k in order:
            load(0, k).start()
        if w == 0:
            for s in small:
                pltpu.make_async_copy(ins[s], bufs[nw + s - nbig], osem.at[s]).wait()
                value = bufs[nw + s - nbig][...]
                if specs[s][1]:
                    value = value * gain_ref[...]
                bufs[s][...] = value.astype(jnp.bfloat16)

        def step(j, carry, w=w, chunk=chunk, steps=steps, scaled=scaled, load=load):
            first = j * chunk
            pending = None
            for k in order:
                load(j, k).wait()
                for c in range(chunk):
                    value = fbuf[k, c]
                    if scaled:
                        value = value * gain_ref[...]
                    bufs[w][k, first + c] = value.astype(jnp.bfloat16)

                @pl.when(j + 1 < steps)
                def _():
                    load(j + 1, k).start()

                if pending is not None:
                    remote(w, pending, bufs[w].at[pending, pl.ds(first, chunk)], first, chunk).start()
                pending = k
            pltpu.make_async_copy(
                bufs[w].at[0, pl.ds(first, chunk)], place(w, me, first, chunk), osem.at[w]
            ).start()
            return carry

        lax.fori_loop(0, steps, step, 0)
        if ntp and w == 0:
            for k in range(1, n):
                token_copy(k, lax.rem(me + n - k, n)).wait()
            own_token_copy().wait()
            for k in range(1, ntp):
                column_copy(k, tp).start()
            pltpu.make_async_copy(cols, column_part(tp), zosem).start()
    for s in small:
        for k in order[:-1]:
            remote(s, k, bufs[s], 0, 0).start()
        pltpu.make_async_copy(bufs[s], place(s, me, 0, 0), osem.at[s]).start()

    for w in range(nw):
        big = w < nbig
        local = outs[w].shape[0] if big else 0
        for k in range(1, n):
            src = bufs[w].at[k] if big else bufs[w]
            source = lax.rem(me + n - k, n)
            pltpu.make_async_remote_copy(
                src_ref=src,
                dst_ref=place(w, source, 0, local),
                send_sem=ssem.at[w, k],
                recv_sem=rsem.at[w, k],
                device_id={"fs": dest[k]},
                device_id_type=MESH,
            ).wait()
        own = bufs[w].at[0] if big else bufs[w]
        pltpu.make_async_copy(own, place(w, me, 0, local), osem.at[w]).wait()
    if ntp:
        for k in range(1, n):
            route_copy(k, lax.rem(me + n - k, n)).wait()
        own_route_copy().wait()
        for k in range(1, ntp):
            column_copy(k, lax.rem(tp + ntp - k, ntp)).wait()
        pltpu.make_async_copy(cols, column_part(tp), zosem).wait()


def exchange(n, ntp, weights, smalls, gain, tokens, collective_id):
    both = weights + smalls
    outs, bufs = [], []
    for a, cut, _ in weights:
        dims = list(a.shape)
        dims[0] //= n
        bufs.append(pltpu.VMEM((n, *dims), jnp.bfloat16))
        dims[cut] *= n
        outs.append(jax.ShapeDtypeStruct(tuple(dims), jnp.bfloat16))
    for a, cut, _ in smalls:
        dims = list(a.shape)
        bufs.append(pltpu.VMEM(tuple(dims), jnp.bfloat16))
        dims[cut] *= n
        outs.append(jax.ShapeDtypeStruct(tuple(dims), jnp.bfloat16))
    for a, _, _ in smalls:
        bufs.append(pltpu.VMEM(a.shape, jnp.float32))
    local = weights[0][0].shape[0] // n
    chunk = 2 if local % 2 == 0 else 1
    sent = sum(2 * a.size * (n - 1) // n for a, _, _ in weights)
    nw = len(both)
    any_spec = pl.BlockSpec(memory_space=pltpu.HBM)
    more, sems = [], []
    if ntp:
        (t, cols), (r, lanes) = tokens[0].shape, tokens[1].shape
        outs += [
            jax.ShapeDtypeStruct((n * t, ntp * cols), jnp.bfloat16),
            jax.ShapeDtypeStruct((n * r, lanes), jnp.float32),
        ]
        sems = [
            pltpu.VMEM((n * t, cols), jnp.bfloat16),
            pltpu.SemaphoreType.DMA((4, n)),
            pltpu.SemaphoreType.DMA((ntp,)),
            pltpu.SemaphoreType.DMA((ntp,)),
            pltpu.SemaphoreType.DMA,
        ]
        more = list(tokens)
    return pl.pallas_call(
        functools.partial(exchange_kernel, n, ntp, [(c, g) for _, c, g in both], len(smalls)),
        out_shape=tuple(outs),
        in_specs=[any_spec] * nw + [pl.BlockSpec(memory_space=pltpu.VMEM)] + [any_spec] * len(more),
        out_specs=(any_spec,) * (nw + len(more)),
        scratch_shapes=[
            pltpu.VMEM((n, chunk, *weights[0][0].shape[1:]), jnp.float32),
            pltpu.SemaphoreType.DMA((n,)),
            pltpu.SemaphoreType.DMA((nw, n)),
            pltpu.SemaphoreType.DMA((nw, n)),
            pltpu.SemaphoreType.DMA((nw,)),
            *bufs,
            *sems,
        ],
        compiler_params=pltpu.CompilerParams(
            collective_id=collective_id, has_side_effects=True, vmem_limit_bytes=60 * 1024 * 1024
        ),
        cost_estimate=pl.CostEstimate(flops=0, bytes_accessed=40 * sent, transcendentals=0),
    )(*[a for a, _, _ in both], gain, *more)


def nt_dot(a, b):
    return lax.dot_general(a, b, (((1,), (1,)), ((), ())), preferred_element_type=jnp.float32)


def up_kernel(
    own_rows, pairs, group, x_ref, route_ref, g_ref, u_ref, sg_ref, su_ref, hid_ref, go_ref, uo_ref, sgo_ref, suo_ref, inv_ref
):
    p = pl.program_id(0)
    rows, d = x_ref.shape
    topk = route_ref.shape[1] // 2
    me = lax.axis_index("fs")

    @pl.when(p == 0)
    def _():
        total = jnp.zeros((rows, 1), jnp.float32)
        width = 512
        for i in range(0, d, width):
            x = x_ref[:, i : i + width].astype(jnp.float32)
            total = total + jnp.sum(x * x, axis=1, keepdims=True)
        inv_ref[...] = jnp.broadcast_to(lax.rsqrt(total / d + norm_eps), inv_ref.shape)
        sgo_ref[...] = sg_ref[...]
        suo_ref[...] = su_ref[...]

    def hidden(g, u):
        acc = nt_dot(x_ref[...], jnp.concatenate([g, u], axis=0))
        half = acc.shape[1] // 2
        gate = acc[:, :half] * inv_ref[:, :1]
        up = acc[:, half:] * inv_ref[:, :1]
        return gate / (1.0 + jnp.exp(-gate)) * up

    @pl.when(p < pairs)
    def _():
        g, u = g_ref[...], u_ref[...]
        go_ref[...] = g
        uo_ref[...] = u
        h = hidden(g.reshape(-1, d), u.reshape(-1, d))
        per = h.shape[1] // group
        lane = lax.broadcasted_iota(jnp.int32, h.shape, 1)
        expert = (me * (group * pairs) + group * p + lane // per).astype(jnp.float32)
        weight = jnp.zeros(h.shape, jnp.float32)
        for k in range(topk):
            weight = weight + jnp.where(
                route_ref[:, k : k + 1] == expert, route_ref[:, topk + k : topk + k + 1], 0.0
            )
        hid_ref[...] = (h * weight).astype(jnp.bfloat16)

    @pl.when(p == pairs)
    def _():
        h = hidden(sg_ref[...], su_ref[...])
        row = lax.broadcasted_iota(jnp.int32, h.shape, 0)
        mine = (row >= me * own_rows) & (row < (me + 1) * own_rows)
        h = jnp.where(mine, h, 0.0).astype(jnp.bfloat16)
        hid_ref[...] = jnp.concatenate([h] + [jnp.zeros_like(h)] * (group - 1), axis=1)


def up_call(own_rows, x, route, gate, up, sg, su):
    experts, hl, d = gate.shape
    group = min(experts, max(1, 128 // hl))
    pairs = experts // group
    rows = x.shape[0]
    whole = pl.BlockSpec(memory_space=pltpu.VMEM)
    pair_spec = pl.BlockSpec((group, hl, d), lambda p: (jnp.minimum(p, pairs - 1), 0, 0))
    return pl.pallas_call(
        functools.partial(up_kernel, own_rows, pairs, group),
        grid=(pairs + 1,),
        out_shape=(
            jax.ShapeDtypeStruct((rows, (pairs + 1) * group * hl), jnp.bfloat16),
            jax.ShapeDtypeStruct(gate.shape, gate.dtype),
            jax.ShapeDtypeStruct(up.shape, up.dtype),
            jax.ShapeDtypeStruct(sg.shape, sg.dtype),
            jax.ShapeDtypeStruct(su.shape, su.dtype),
        ),
        in_specs=[whole, whole, pair_spec, pair_spec, whole, whole],
        out_specs=(
            pl.BlockSpec((rows, group * hl), lambda p: (0, p)),
            pair_spec,
            pair_spec,
            whole,
            whole,
        ),
        scratch_shapes=[pltpu.VMEM((rows, 128), jnp.float32)],
        compiler_params=pltpu.CompilerParams(vmem_limit_bytes=60 * 1024 * 1024),
        cost_estimate=pl.CostEstimate(
            flops=4 * rows * d * hl * (experts + 1), bytes_accessed=8 * gate.size, transcendentals=0
        ),
    )(x, route, gate, up, sg, su)


def down_kernel(hid_ref, d_ref, sd_ref, out_ref, do_ref, sdo_ref, acc_ref):
    i = pl.program_id(0)
    d = d_ref[...]
    do_ref[...] = d
    sd = sd_ref[...]
    sdo_ref[...] = sd
    hl = sd.shape[0]
    wide = d.shape[0] * hl
    total = jnp.dot(hid_ref[0, :, :wide], d.reshape(wide, -1), preferred_element_type=jnp.float32)
    total += jnp.dot(hid_ref[0, :, wide : wide + hl], sd, preferred_element_type=jnp.float32)

    @pl.when(i == 0)
    def _():
        acc_ref[...] = total

    @pl.when(i > 0)
    def _():
        acc_ref[...] += total

    @pl.when(i == pl.num_programs(0) - 1)
    def _():
        out_ref[...] = acc_ref[...].astype(jnp.bfloat16)


def down_call(hid, down, sd):
    parts, rows, lanes = hid.shape
    experts, h, d = down.shape
    hl = h // parts
    d_spec = pl.BlockSpec((experts, hl, d), lambda i: (0, i, 0))
    sd_spec = pl.BlockSpec((hl, d), lambda i: (i, 0))
    return pl.pallas_call(
        down_kernel,
        grid=(parts,),
        out_shape=(
            jax.ShapeDtypeStruct((rows, d), jnp.bfloat16),
            jax.ShapeDtypeStruct(down.shape, down.dtype),
            jax.ShapeDtypeStruct(sd.shape, sd.dtype),
        ),
        in_specs=[pl.BlockSpec((1, rows, lanes), lambda i: (i, 0, 0)), d_spec, sd_spec],
        out_specs=(pl.BlockSpec((rows, d), lambda i: (0, 0)), d_spec, sd_spec),
        scratch_shapes=[pltpu.VMEM((rows, d), jnp.float32)],
        compiler_params=pltpu.CompilerParams(vmem_limit_bytes=60 * 1024 * 1024),
        cost_estimate=pl.CostEstimate(flops=2 * rows * d * experts * h, bytes_accessed=6 * down.size, transcendentals=0),
    )(hid, down, sd)


def combine_kernel(n, part_ref, out_ref, landed, ssem, rsem):
    me = lax.axis_index("fs")
    rows = out_ref.shape[0]
    barrier = pltpu.get_barrier_semaphore()
    for k in range(1, n):
        pl.semaphore_signal(barrier, inc=1, device_id={"fs": lax.rem(me + k, n)}, device_id_type=MESH)
    pl.semaphore_wait(barrier, n - 1)

    def block(who):
        return part_ref.at[pl.ds(pl.multiple_of(who * rows, rows), rows)]

    copies = []
    for k in range(1, n):
        to = lax.rem(me + k, n)
        copy = pltpu.make_async_remote_copy(
            src_ref=block(to),
            dst_ref=landed.at[k - 1],
            send_sem=ssem.at[k - 1],
            recv_sem=rsem.at[k - 1],
            device_id={"fs": to},
            device_id_type=MESH,
        )
        copy.start()
        copies.append(copy)
    total = block(me)[...].astype(jnp.float32)
    for k in range(1, n):
        copies[k - 1].wait()
        total = total + landed[k - 1].astype(jnp.float32)
    out_ref[...] = total.astype(out_ref.dtype)


def combine(n, part, collective_id):
    rows, d = part.shape[0] // n, part.shape[1]
    vmem = pl.BlockSpec(memory_space=pltpu.VMEM)
    return pl.pallas_call(
        functools.partial(combine_kernel, n),
        out_shape=jax.ShapeDtypeStruct((rows, d), part.dtype),
        in_specs=[vmem],
        out_specs=vmem,
        scratch_shapes=[
            pltpu.VMEM((n - 1, rows, d), part.dtype),
            pltpu.SemaphoreType.DMA((n - 1,)),
            pltpu.SemaphoreType.DMA((n - 1,)),
        ],
        compiler_params=pltpu.CompilerParams(collective_id=collective_id, has_side_effects=True, vmem_limit_bytes=60 * 1024 * 1024),
    )(part)


def body(
    n,
    ntp,
    tokens,
    expert_ids,
    affinity,
    norm_gain,
    gate_train,
    up_train,
    down_train,
    shared_gate_train,
    shared_up_train,
    shared_down_train,
):
    own_rows = tokens.shape[0]
    route_weight = routed_scale * affinity / jnp.sum(affinity, axis=1, keepdims=True)
    route = jnp.concatenate([expert_ids.astype(jnp.float32), route_weight], axis=1)
    gain = norm_gain[None, :]
    gate, up, sg, su, sd, x, route = exchange(
        n,
        ntp,
        [(gate_train, 2, True), (up_train, 2, True)],
        [(shared_gate_train, 1, True), (shared_up_train, 1, True), (shared_down_train, 0, False)],
        gain,
        (tokens, route),
        0,
    )
    hid, gate_serve, up_serve, shared_gate_serve, shared_up_serve = up_call(own_rows, x, route, gate, up, sg, su)
    down_in, hid = lax.optimization_barrier((down_train, hid))
    every = lax.all_gather(hid, "tp", axis=0)
    (down,) = exchange(n, 0, [(down_in, 1, False)], [], gain, None, 1)
    part, down_serve, shared_down_serve = down_call(every, down, sd)
    mixed = combine(n, part, 2)
    return (
        mixed,
        gate_serve,
        up_serve,
        down_serve,
        shared_gate_serve,
        shared_up_serve,
        shared_down_serve,
    )


def solution(mesh):
    return jax.shard_map(
        functools.partial(body, mesh.shape["fs"], mesh.shape["tp"]),
        mesh=mesh,
        in_specs=(
            P("fs", "tp"),
            P("fs", None),
            P("fs", None),
            P("fs"),
            P(None, "tp", "fs"),
            P(None, "tp", "fs"),
            P(None, "fs", "tp"),
            P("tp", "fs"),
            P("tp", "fs"),
            P("fs", "tp"),
        ),
        out_specs=(
            P("fs", "tp"),
            P("fs", "tp", None),
            P("fs", "tp", None),
            P("fs", None, "tp"),
            P("tp", None),
            P("tp", None),
            P(None, "tp"),
        ),
        check_vma=False,
    )
```
